32 devices in a mesh: grp: 2 (over y), sp: 4 (over z), dp: 4 (over x, core).
Axes of the slice: x: 2, y: 2, z: 4, core: 2. Of those that a mesh axis runs over, the one named last changes fastest.
Arguments:
- query_rows: bfloat16 [8, 512, 2048], P(('grp', 'dp'), 'sp'), parts along dimension 0, may hold values from -6 to 6
- key_rows: bfloat16 [8, 512, 2048], P(('grp', 'dp'), 'sp'), parts along dimension 0, may hold values from -6 to 6
- value_rows: bfloat16 [8, 512, 2048], P(('grp', 'dp'), 'sp'), parts along dimension 0, may hold values from -6 to 6
- query_gain: float32 [64], replicated, may hold values from 1.1 to 7
- key_gain: float32 [64], replicated, may hold values from 1.1 to 7
- lambdas: float32 [16], replicated, may hold values from 0.3 to 0.8
- head_gain: float32 [128], replicated, may hold values from 0.1 to 1.9
- out_weight: bfloat16 [2048, 2048], P(None, 'dp'), may hold values from -0.125 to 0.125
Outputs:
- attended: bfloat16 [8, 512, 2048], P(('grp', 'dp'), 'sp'), parts along dimension 0
The draws below stay inside these ranges and needn't reach their ends.
There are 2 independent parts, one for each index of `grp`. The reference program is written for one: setup_inputs(seed, part) draws one part's arguments, and reference() takes and returns one part's arrays. A program takes and returns all parts, laid end to end along the dimension named above; an argument that names none is the same for every part. Nothing has to cross between parts.
All inputs are finite; a program needn't handle non-finite values.
Results may differ from the reference program's by a relative error of at most 0.008.
The reference program's roundings to bfloat16 on the way count: a program that leaves them out, or rounds other values in their place, can miss the bound.
Values may be sent and summed in bfloat16 or wider, within the bound.
No kernel may reach another device: no remote copies, remote signals or barrier semaphores. Data moves between devices by JAX's collectives and lax.ppermute only.
A program may use at most 128 MiB of HBM per device.

```python
import jax
import jax.numpy as jnp
from jax import lax

D = 2048
HEADS = 16
HEAD = 64
VDIM = 128
LENGTH = 512
SEQS = 4


def paired_rows(key):
    shape = (SEQS, LENGTH, HEADS * 2 * HEAD)
    key_part = jnp.clip(jax.random.normal(jax.random.fold_in(key, 101), shape, jnp.float32), -6.0, 6.0)
    query_part = jnp.clip(jax.random.normal(jax.random.fold_in(key, 202), shape, jnp.float32), -6.0, 6.0)
    return (query_part, key_part)


def draw_query_rows(key, part):
    return paired_rows(key)[0].astype(jnp.bfloat16)


def draw_key_rows(key, part):
    return paired_rows(key)[1].astype(jnp.bfloat16)


def gain_draw(key):
    return jax.random.uniform(key, (HEAD,), jnp.float32, 1.1, 1.7)


def draw_query_gain(key, part):
    return gain_draw(jax.random.fold_in(key, 31))


def draw_key_gain(key, part):
    return gain_draw(jax.random.fold_in(key, 32))


def shard_levels(key, shape, cuts, smallest, largest):
    level, own = 1.0, jax.random.fold_in(key, 6)
    for dim, shards_of in cuts:
        steps = jnp.exp(jax.random.uniform(jax.random.fold_in(own, dim), (shards_of,), jnp.float32, smallest / len(cuts), largest / len(cuts)))
        level = level * jnp.repeat(steps, shape[dim] // shards_of).reshape([-1 if axis == dim else 1 for axis in range(len(shape))])
    return level


def noise(rng, shape, scale, limit, split=(), kind=jnp.bfloat16):
    factor_of = shard_levels(rng, shape, split, -0.22, 0.18) if split else 1.0
    values = jax.random.normal(rng, shape, jnp.float32) * scale * factor_of
    return jnp.minimum(jnp.maximum(values, -limit), limit).astype(kind)


def setup_inputs(seed: int = 0, part: int = 0) -> dict:
    key_of = jax.random.split(jax.random.key(seed), 9)
    own_keys = jax.random.split(jax.random.fold_in(key_of[8], part), 9)
    query_rows = draw_query_rows(jax.random.fold_in(jax.random.fold_in(key_of[8], part), 71), part)
    key_rows = draw_key_rows(jax.random.fold_in(jax.random.fold_in(key_of[8], part), 71), part)
    value_rows = noise(own_keys[2], (SEQS, LENGTH, HEADS * VDIM), 1.0, 6.0, ((0, 4), (1, 4)))
    query_gain = draw_query_gain(jax.random.fold_in(key_of[8], 71), part)
    key_gain = draw_key_gain(jax.random.fold_in(key_of[8], 71), part)
    lambdas = jnp.clip(jax.random.uniform(key_of[5], (HEADS,), jnp.float32, 0.3, 0.8), 0.3, 0.8)
    head_gain = jnp.clip(1.0 + 0.18 * jax.random.normal(key_of[6], (VDIM,), jnp.float32), 0.1, 1.9)
    out_weight = noise(key_of[7], (HEADS * VDIM, D), (HEADS * VDIM) ** -0.5, 0.125, ((1, 4),))
    return {"query_rows": query_rows, "key_rows": key_rows, "value_rows": value_rows, "query_gain": query_gain, "key_gain": key_gain, "lambdas": lambdas, "head_gain": head_gain, "out_weight": out_weight}


EPSILON = 1e-06
OUT_SCALE = 0.8

def norm_rotate(field_rows, gain_vector, positions):
    widened = field_rows.astype(jnp.float32)
    normed = widened * lax.rsqrt(lax.optimization_barrier(jnp.mean(widened * widened, axis=-1, keepdims=True)) + EPSILON) * gain_vector
    half_size = field_rows.shape[-1] // 2
    inverse = 10000.0 ** (-jnp.arange(half_size, dtype=jnp.float32) / half_size)
    angles = (positions[:, None] * inverse[None, :]).reshape(positions.shape[0], 1, 1, half_size)
    cosine_part = jnp.cos(angles)
    sine_part = jnp.sin(angles)
    first_half = normed[..., :half_size]
    second_half = normed[..., half_size:]
    turned = jnp.concatenate([first_half * cosine_part - second_half * sine_part, second_half * cosine_part + first_half * sine_part], axis=-1)
    return turned.astype(jnp.bfloat16)

def head_norm(raw_heads, gain_vector):
    scaled = raw_heads * lax.rsqrt(lax.optimization_barrier(jnp.mean(raw_heads * raw_heads, axis=-1, keepdims=True)) + EPSILON)
    return (scaled * gain_vector * OUT_SCALE).astype(jnp.bfloat16)

def block_size(length):
    return 512 if length % 512 == 0 else length

def attend(query_head, key_head, value_head, weight_two, gain_vector):
    length = query_head.shape[0]
    block_rows = block_size(length)
    score_scale = query_head.shape[-1] ** (-0.5)
    key_wide = key_head.astype(jnp.float32)
    key_positions = jnp.arange(length, dtype=jnp.int32)

    def one_block(number):
        first_row = number * block_rows
        query_block = lax.dynamic_slice_in_dim(query_head, first_row, block_rows, 0).astype(jnp.float32)
        scores = jnp.einsum('qcd,kcd->cqk', query_block, key_wide) * score_scale
        query_positions = first_row + jnp.arange(block_rows, dtype=jnp.int32)
        visible = key_positions[None, :] <= query_positions[:, None]
        scores = jnp.where(visible[None], scores, -1e+30)
        highest = lax.optimization_barrier(jnp.max(scores, axis=-1, keepdims=True))
        exponent = jnp.exp(scores - highest)
        probabilities = exponent / lax.optimization_barrier(jnp.sum(exponent, axis=-1, keepdims=True))
        mixing = (probabilities[0] - weight_two * probabilities[1]).astype(jnp.bfloat16)
        return jnp.dot(mixing, value_head, preferred_element_type=jnp.float32)
    blocks = lax.map(one_block, jnp.arange(length // block_rows, dtype=jnp.int32))
    return head_norm(blocks.reshape(length, value_head.shape[-1]), gain_vector)

def reference(query_rows, key_rows, value_rows, query_gain, key_gain, lambdas, head_gain, out_weight):
    seq_count = query_rows.shape[0]
    length = query_rows.shape[1]
    positions = jnp.arange(length, dtype=jnp.float32)
    query_rot = norm_rotate(query_rows.reshape(seq_count, length, HEADS, 2, HEAD), query_gain, positions)
    key_rot = norm_rotate(key_rows.reshape(seq_count, length, HEADS, 2, HEAD), key_gain, positions)
    value_heads = value_rows.reshape(seq_count, length, HEADS, VDIM)

    def per_item(number):
        seq_index = number // HEADS
        head_index = number % HEADS
        return attend(query_rot[seq_index, :, head_index], key_rot[seq_index, :, head_index], value_heads[seq_index, :, head_index], lambdas[head_index], head_gain)
    outputs = lax.map(per_item, jnp.arange(seq_count * HEADS, dtype=jnp.int32))
    outputs = outputs.reshape(seq_count, HEADS, length, VDIM).transpose(0, 2, 1, 3)
    outputs = outputs.reshape(seq_count * length, HEADS * VDIM)
    attended = jnp.dot(outputs, out_weight, preferred_element_type=jnp.float32).astype(jnp.bfloat16)
    return attended.reshape(seq_count, length, out_weight.shape[1])
```

```python
import functools
import math

import jax
import jax.numpy as jnp
import numpy as np
from jax import lax
from jax.experimental import pallas as pl
from jax.experimental.pallas import tpu as pltpu
from jax.sharding import PartitionSpec as P

EPSILON = 1e-06
OUT_SCALE = 0.8
CHUNK_PARTS = (4, 4)


def pack_flows(flows):
    rounds = []
    for flow in flows:
        for members in rounds:
            if all(flow[0] != other[0] and flow[1] != other[1] for other in members):
                members.append(flow)
                break
        else:
            rounds.append([flow])
    return rounds


class Plan:
    def __init__(self, n):
        self.n = n
        self.owners = sorted({max(n // 2 - 1, 0), n // 2})
        with_queries, keys_values, back = [], [], []
        for group, owner in enumerate(self.owners):
            for block in range(owner + 1, n):
                with_queries.append((block, owner, group))
                back.append((owner, block, group))
            for block in range(owner):
                for target in range(block + 1, owner + 1):
                    keys_values.append((block, target, group))
        self.ins = [(3, members) for members in pack_flows(with_queries)]
        self.ins += [(2, members) for members in pack_flows(keys_values)]
        self.outs = pack_flows(back)
        table = np.full((n, 3 * (len(self.ins) + len(self.outs)) + 1), -1, np.int32)
        for number, (_, members) in enumerate(self.ins):
            for source, target, group in members:
                table[source, 3 * number] = group
                table[target, 3 * number + 1] = group
                table[target, 3 * number + 2] = source
        for number, members in enumerate(self.outs):
            place = 3 * (len(self.ins) + number)
            for source, target, group in members:
                table[source, place] = group
                table[source, place + 1] = target
                table[target, place + 2] = group
        self.table = table

    def in_entry(self, table, me, number):
        return [table[me, 3 * number + part] for part in range(3)]

    def out_entry(self, table, me, number):
        return [table[me, 3 * (len(self.ins) + number) + part] for part in range(3)]


SMEM_SPEC = pl.BlockSpec(memory_space=pltpu.SMEM)
HBM_SPEC = pl.BlockSpec(memory_space=pltpu.HBM)
VMEM_SPEC = pl.BlockSpec(memory_space=pltpu.VMEM)


def send_buffers(plan, table, rows, first_head, chunk_heads, group_heads, width):
    def body(table_ref, query_ref, key_ref, value_ref, *rest):
        buffers, sems = rest[: len(plan.ins)], rest[len(plan.ins)]
        me = lax.axis_index("sp")
        for start in (True, False):
            count = 0
            for number, (parts, _) in enumerate(plan.ins):
                group = plan.in_entry(table_ref, me, number)[0]
                arrays = (query_ref, key_ref, value_ref)[3 - parts :]
                column = pl.multiple_of((jnp.maximum(group, 0) * group_heads + first_head) * width, width)

                @pl.when(group >= 0)
                def _(arrays=arrays, number=number, column=column, count=count):
                    for part, array in enumerate(arrays):
                        copy = pltpu.make_async_copy(
                            array.at[:, pl.ds(column, chunk_heads * width)],
                            buffers[number].at[part],
                            sems.at[count + part],
                        )
                        copy.start() if start else copy.wait()

                count += parts

    tokens = rows[0].shape[0]
    shapes = [
        jax.ShapeDtypeStruct((parts, tokens, chunk_heads * width), rows[0].dtype)
        for parts, _ in plan.ins
    ]
    return pl.pallas_call(
        body,
        out_shape=shapes,
        in_specs=[SMEM_SPEC] + [HBM_SPEC] * 3,
        out_specs=[HBM_SPEC] * len(shapes),
        scratch_shapes=[pltpu.SemaphoreType.DMA((sum(parts for parts, _ in plan.ins),))],
        name="pack",
    )(table, *rows)


def attention(plan, table, rows, arrived, tables, gains, lambdas, head_gain, first_head, chunk_heads, group_heads):
    n, groups = plan.n, len(plan.owners)
    tokens = rows[0].shape[0]
    width = head_gain.shape[-1]
    half = width // 2
    length = n * tokens
    both = 2 if chunk_heads % 2 == 0 and first_head % 2 == 0 and group_heads % 2 == 0 else 1
    steps = chunk_heads // both
    segment = max(1, n // 4)
    sizes = sorted({min(n, start + segment) for start in range(0, n, segment)})
    exponent_scale = half ** (-0.5) * math.log2(math.e)

    def body(table_ref, lambda_ref, gains_ref, head_gain_ref, cos_ref, sin_ref, *rest):
        own_refs, rest = rest[: 3 * groups], rest[3 * groups :]
        in_refs, rest = rest[: len(plan.ins)], rest[len(plan.ins) :]
        own_out, rest = rest[0], rest[1:]
        outs, rest = rest[: len(plan.outs)], rest[len(plan.outs) :]
        query_rot, key_rot, value_all, result = rest
        me = lax.axis_index("sp")
        step = pl.program_id(0)

        row = lax.broadcasted_iota(jnp.int32, (width, width), 0)
        column = lax.broadcasted_iota(jnp.int32, (width, width), 1)
        same_map = row // half == column // half
        sum_matrix = same_map.astype(jnp.bfloat16)
        sum_twice = jnp.concatenate([sum_matrix, sum_matrix], axis=0)
        pair_matrix = (same_map & (jnp.abs(row - column) == half // 2)).astype(jnp.bfloat16)

        def rotate(field, slot, which):
            wide = field.astype(jnp.float32)
            square = wide * wide
            high = square.astype(jnp.bfloat16)
            low = (square - high.astype(jnp.float32)).astype(jnp.bfloat16)
            total = jnp.dot(
                jnp.concatenate([high, low], axis=1), sum_twice, preferred_element_type=jnp.float32
            )
            pair = jnp.dot(field, pair_matrix, preferred_element_type=jnp.float32)
            here = pl.ds(pl.multiple_of(slot * tokens, tokens), tokens)
            turned = wide * (cos_ref[here, :] * gains_ref[which : which + 1, :])
            turned += pair * (sin_ref[here, :] * gains_ref[which + 1 : which + 2, :])
            return (turned * lax.rsqrt(total * (1.0 / half) + EPSILON)).astype(jnp.bfloat16)

        def place(group, slot, query, key, value):
            here = pl.ds(pl.multiple_of(slot * tokens, tokens), tokens)
            for head in range(both):
                lanes = slice(head * width, (head + 1) * width)
                if query is not None:
                    query_rot[group, head, here, :] = rotate(query[..., lanes], slot, 0)
                key_rot[group, head, here, :] = rotate(key[..., lanes], slot, 2)
                value_all[group, head, here, :] = value[..., lanes]

        if segment > 1:

            @pl.when(step == 0)
            def _():
                value_all[...] = jnp.zeros_like(value_all)

        for group, owner in enumerate(plan.owners):

            @pl.when(me <= owner)
            def _(group=group):
                place(group, me, *(ref[...] for ref in own_refs[3 * group : 3 * group + 3]))

        for number, (parts, _) in enumerate(plan.ins):
            _, group, slot = plan.in_entry(table_ref, me, number)

            @pl.when(group >= 0)
            def _(number=number, parts=parts, group=group, slot=slot):
                fields = [in_refs[number][part] for part in range(parts)]
                place(group, slot, *([None] * (3 - parts) + fields))

        def job(number, carry):
            group = number // n
            offset = number - group * n
            owner = jnp.int32(plan.owners[0])
            for other in range(1, groups):
                owner = jnp.where(group == other, plan.owners[other], owner)
            block = me + offset
            active = jnp.where(me == owner, block < n, (me < owner) & (offset == 0))
            here = pl.ds(pl.multiple_of(jnp.minimum(block, n - 1) * tokens, tokens), tokens)

            def compute(size):
                first_map = lax.broadcasted_iota(jnp.int32, (tokens, width), 1) < half
                key_at = lax.broadcasted_iota(jnp.int32, (2 * tokens, segment * tokens), 1)
                query_at = lax.broadcasted_iota(jnp.int32, (2 * tokens, segment * tokens), 0) % tokens
                visible = key_at + (size - segment) * tokens <= query_at + block * tokens
                for head in range(both):
                    query = query_rot[group, head, here, :]
                    zero = jnp.zeros_like(query)
                    maps = jnp.concatenate(
                        [jnp.where(first_map, query, zero), jnp.where(first_map, zero, query)], axis=0
                    )
                    scores = lax.dot_general(
                        maps,
                        key_rot[group, head, : size * tokens, :],
                        (((1,), (1,)), ((), ())),
                        preferred_element_type=jnp.float32,
                    )
                    border = (size - segment) * tokens
                    last = jnp.where(visible, scores[:, border:], -1e30)
                    scores = jnp.concatenate([scores[:, :border], last], axis=1) if border else last
                    highest = jnp.max(scores, axis=1, keepdims=True)
                    exponent = jnp.exp2((scores - highest) * exponent_scale)
                    inverse = 1.0 / jnp.sum(exponent, axis=1, keepdims=True)
                    weight = lambda_ref[group * group_heads + first_head + step * both + head]
                    mixing = (
                        exponent[:tokens] * inverse[:tokens]
                        - exponent[tokens:] * (inverse[tokens:] * weight)
                    ).astype(jnp.bfloat16)
                    raw = jnp.dot(
                        mixing,
                        value_all[group, head, : size * tokens, :],
                        preferred_element_type=jnp.float32,
                    )
                    scaled = raw * lax.rsqrt(jnp.mean(raw * raw, axis=1, keepdims=True) + EPSILON)
                    result[:, head * width : (head + 1) * width] = (
                        scaled * (head_gain_ref[...] * OUT_SCALE)
                    ).astype(jnp.bfloat16)

            low = 0
            for size in sizes:
                pl.when(active & (block >= low) & (block < size))(functools.partial(compute, size))
                low = size

            @pl.when(active & (offset == 0))
            def _():
                own_out[group] = result[...]

            for place_number in range(len(plan.outs)):
                send_group, send_block, _ = plan.out_entry(table_ref, me, place_number)

                @pl.when(active & (send_group == group) & (send_block == block))
                def _(place_number=place_number):
                    outs[place_number][...] = result[...]

            return carry

        lax.fori_loop(0, groups * n, job, 0)

    def whole(shape):
        return pl.BlockSpec(shape, lambda s: (0,) * len(shape))

    own_specs, own_args = [], []
    for group in range(groups):
        offset = (group * group_heads + first_head) // both
        for array in rows:
            own_specs.append(pl.BlockSpec((tokens, both * width), lambda s, offset=offset: (0, offset + s)))
            own_args.append(array)
    in_specs = [SMEM_SPEC, SMEM_SPEC, whole(gains.shape), whole(head_gain.shape)]
    in_specs += [whole(tables[0].shape), whole(tables[1].shape)] + own_specs
    in_specs += [
        pl.BlockSpec((parts, tokens, both * width), lambda s: (0, 0, s)) for parts, _ in plan.ins
    ]
    columns = chunk_heads * width
    out_shape = [jax.ShapeDtypeStruct((groups, tokens, columns), jnp.bfloat16)]
    out_shape += [jax.ShapeDtypeStruct((tokens, columns), jnp.bfloat16)] * len(plan.outs)
    out_specs = [pl.BlockSpec((groups, tokens, both * width), lambda s: (0, 0, s))]
    out_specs += [pl.BlockSpec((tokens, both * width), lambda s: (0, s))] * len(plan.outs)
    results = pl.pallas_call(
        body,
        grid=(steps,),
        out_shape=out_shape,
        in_specs=in_specs,
        out_specs=out_specs,
        scratch_shapes=[pltpu.VMEM((groups, both, length, width), jnp.bfloat16)] * 3
        + [pltpu.VMEM((tokens, both * width), jnp.bfloat16)],
        name="attend",
    )(table, lambdas, gains, head_gain, *tables, *own_args, *arrived)
    return results[0], results[1:]


def project(plan, table, own_heads, back, shards, total, first_head, chunk_heads, group_heads, last, dtype):
    groups, tokens, columns = own_heads.shape
    shard_columns = shards[0].shape[1]
    width = columns // chunk_heads
    count = len(shards)
    given = 0 if total is None else 1

    def body(table_ref, own_ref, *rest):
        back_refs, rest = rest[: len(plan.outs)], rest[len(plan.outs) :]
        total_refs, rest = rest[:given], rest[given:]
        shard_refs, rest = rest[:count], rest[count:]
        out_ref, weight, heads, sems = rest
        me, column_place = lax.axis_index("sp"), lax.axis_index("dp")

        def copy(number, group):
            row = (group * group_heads + first_head) * width
            return pltpu.make_async_copy(
                shard_refs[number].at[pl.ds(row, columns), :],
                weight.at[number, pl.ds(group * columns, columns), :],
                sems.at[number, group],
            )

        for number in range(count):
            for group in range(groups):
                copy(number, group).start()
        for group, owner in enumerate(plan.owners):
            lanes = slice(group * columns, (group + 1) * columns)

            @pl.when(me <= owner)
            def _(group=group, lanes=lanes):
                heads[:, lanes] = own_ref[group]

            for number in range(len(plan.outs)):
                _, _, from_group = plan.out_entry(table_ref, me, number)

                @pl.when(from_group == group)
                def _(number=number, lanes=lanes):
                    heads[:, lanes] = back_refs[number][...]

        for number in range(count):
            for group in range(groups):
                copy(number, group).wait()
            part = jnp.dot(heads[...], weight[number], preferred_element_type=jnp.float32)
            if given:
                part += total_refs[0][number]
            if last:
                column = pl.multiple_of(shard_place(column_place, number, count) * shard_columns, shard_columns)
                out_ref[:, pl.ds(column, shard_columns)] = part.astype(dtype)
            else:
                out_ref[number] = part

    if last:
        out_shape = jax.ShapeDtypeStruct((tokens, count * shard_columns), dtype)
    else:
        out_shape = jax.ShapeDtypeStruct((count, tokens, shard_columns), jnp.float32)
    return pl.pallas_call(
        body,
        out_shape=out_shape,
        in_specs=[SMEM_SPEC] + [VMEM_SPEC] * (1 + len(plan.outs) + given) + [HBM_SPEC] * count,
        out_specs=VMEM_SPEC,
        scratch_shapes=[
            pltpu.VMEM((count, groups * columns, shard_columns), jnp.bfloat16),
            pltpu.VMEM((tokens, groups * columns), jnp.bfloat16),
            pltpu.SemaphoreType.DMA((count, groups)),
        ],
        name="project",
    )(table, own_heads, *back, *([] if total is None else [total]), *shards)


def shard_place(place, number, count):
    if count & (count - 1) == 0:
        return jnp.bitwise_xor(place, number)
    return lax.rem(place + number, count)


def gather_shards(weight):
    count = lax.axis_size("dp")
    if count & (count - 1):
        return [weight] + [
            lax.ppermute(weight, "dp", [(j, (j - k) % count) for j in range(count)])
            for k in range(1, count)
        ]
    shards, mask = {0: weight}, count // 2
    while mask:
        pairs = [(j, j ^ mask) for j in range(count)]
        shards.update({k ^ mask: lax.ppermute(shard, "dp", pairs) for k, shard in shards.items()})
        mask //= 2
    return [shards[k] for k in range(count)]


def rotation_tables(length, head_size):
    half_size = head_size // 2
    positions = jnp.arange(length, dtype=jnp.float32)
    inverse = 10000.0 ** (-jnp.arange(half_size, dtype=jnp.float32) / half_size)
    angles = positions[:, None] * inverse[None, :]
    cosine_part, sine_part = jnp.cos(angles), jnp.sin(angles)
    return (
        jnp.concatenate([cosine_part] * 4, axis=1),
        jnp.concatenate([-sine_part, sine_part] * 2, axis=1),
    )


def local(query_rows, key_rows, value_rows, query_gain, key_gain, lambdas, head_gain, out_weight):
    tokens = query_rows.shape[1]
    plan = Plan(lax.axis_size("sp"))
    heads_total = lambdas.shape[0]
    group_heads = heads_total // len(plan.owners)
    head_size, width = query_gain.shape[0], head_gain.shape[0]
    length = tokens * plan.n
    table = jnp.asarray(plan.table)
    rows = [array.reshape(tokens, array.shape[2]) for array in (query_rows, key_rows, value_rows)]

    bounds = [group_heads * sum(CHUNK_PARTS[:k]) // sum(CHUNK_PARTS) for k in range(len(CHUNK_PARTS) + 1)]
    chunks = [(start, stop - start) for start, stop in zip(bounds, bounds[1:]) if stop > start]

    arrived = []
    for first_head, chunk_heads in chunks:
        buffers = send_buffers(plan, table, rows, first_head, chunk_heads, group_heads, width)
        arrived.append(
            [
                lax.ppermute(buffer, "sp", [flow[:2] for flow in members])
                for buffer, (_, members) in zip(buffers, plan.ins)
            ]
        )
    shards = gather_shards(out_weight)
    tables = rotation_tables(length, head_size)
    swapped = [jnp.roll(gain, head_size // 2) for gain in (query_gain, key_gain)]
    gains = jnp.stack(
        [jnp.tile(gain, 2) for gain in (query_gain, swapped[0], key_gain, swapped[1])]
    )
    total = None
    for number, (first_head, chunk_heads) in enumerate(chunks):
        own_heads, outward = attention(
            plan, table, rows, arrived[number], tables, gains, lambdas, head_gain.reshape(1, width),
            first_head, chunk_heads, group_heads,
        )
        back = [
            lax.ppermute(buffer, "sp", [flow[:2] for flow in members])
            for buffer, members in zip(outward, plan.outs)
        ]
        total = project(
            plan, table, own_heads, back, shards, total, first_head, chunk_heads, group_heads,
            number == len(chunks) - 1, query_rows.dtype,
        )
    return total.reshape(1, tokens, total.shape[1])


def solution(mesh):
    placed = (
        P(("grp", "dp"), "sp", None),
        P(("grp", "dp"), "sp", None),
        P(("grp", "dp"), "sp", None),
        P(),
        P(),
        P(),
        P(),
        P(None, "dp"),
    )
    return jax.shard_map(
        local, mesh=mesh, in_specs=placed, out_specs=P(("grp", "dp"), "sp", None), check_vma=False
    )
```

```python
import functools
import math

import jax
import jax.numpy as jnp
import numpy as np
from jax import lax
from jax.experimental import pallas as pl
from jax.experimental.pallas import tpu as pltpu
from jax.sharding import PartitionSpec as P

EPSILON = 1e-06
OUT_SCALE = 0.8
CHUNK_PARTS = (1, 1)
FIRST_GROUP = 3 / 8
MIB = 1024 * 1024


VMEM_SPEC = pl.BlockSpec(memory_space=pltpu.VMEM)
HBM_SPEC = pl.BlockSpec(memory_space=pltpu.HBM)
SMEM_SPEC = pl.BlockSpec(memory_space=pltpu.SMEM)
QUERY, KEY, VALUE = range(3)


class Plan:
    def __init__(self, n, owners, heads):
        self.n, self.owners, self.heads = n, owners, heads
        inward, back = {}, {}
        self.jobs = {device: [] for device in range(n)}
        for group, owner in enumerate(owners):
            for block in range(n):
                self.jobs[min(block, owner)].append((group, block))
                if block > owner:
                    inward.setdefault((block, owner), []).append((group, QUERY))
                    back.setdefault((owner, block), []).append(group)
                for target in range(block + 1, owner + 1):
                    inward.setdefault((block, target), []).append((group, KEY))
        self.ins = self.rounds(inward, lambda part: (3 - part[1]) * heads[part[0]])
        self.outs = self.rounds(back, lambda group: heads[group])

    def rounds(self, flows, slabs):
        sized = sorted(flows.items(), key=lambda flow: -sum(map(slabs, flow[1])))
        rounds = []
        for (source, target), parts in sized:
            places, count = [], 0
            for part in parts:
                places.append((part, count))
                count += slabs(part)
            for members in rounds:
                if all(source != other[0] and target != other[1] for other in members[1]):
                    members[1].append((source, target, places))
                    break
            else:
                rounds.append((count, [(source, target, places)]))
        return rounds

    def source_of(self, rounds, source, target, wanted):
        for number, (_, members) in enumerate(rounds):
            for member_source, member_target, places in members:
                if (member_source, member_target) == (source, target):
                    for part, first in places:
                        if part == wanted:
                            return number, first
        raise KeyError(wanted)


def pairs_of(members):
    return [(source, target) for source, target, _ in members]


def send_buffers(plan, rows, tables, gains, first_heads, width):
    groups = len(plan.owners)
    tokens = rows[0].shape[0]
    half = width // 2

    def body(*refs):
        row_refs, refs = refs[:3], refs[3:]
        cos_table, sin_table, query_gain_ref, key_gain_ref, *refs = refs
        own, refs = refs[:groups], refs[groups:]
        buffers, refs = refs[: len(plan.ins)], refs[len(plan.ins) :]
        staged, (cos_here, sin_here, query_gain, key_gain, sems) = refs[:groups], refs[groups:]
        me = lax.axis_index("sp")
        here = pl.ds(pl.multiple_of(me * tokens, tokens), tokens)
        copies = [
            pltpu.make_async_copy(cos_table.at[here, :], cos_here, sems.at[0]),
            pltpu.make_async_copy(sin_table.at[here, :], sin_here, sems.at[1]),
            pltpu.make_async_copy(query_gain_ref, query_gain, sems.at[2]),
            pltpu.make_async_copy(key_gain_ref, key_gain, sems.at[3]),
        ]
        for group in range(groups):
            lanes = pl.ds(first_heads[group] * width, plan.heads[group] * width)
            for part in range(3):
                copies.append(
                    pltpu.make_async_copy(
                        row_refs[part].at[:, lanes], staged[group].at[part], sems.at[len(copies)]
                    )
                )
        for copy in copies:
            copy.start()

        row = lax.broadcasted_iota(jnp.int32, (width, width), 0)
        column = lax.broadcasted_iota(jnp.int32, (width, width), 1)
        same_map = row // half == column // half
        sum_matrix = same_map.astype(jnp.bfloat16)
        sum_twice = jnp.concatenate([sum_matrix, sum_matrix], axis=0)
        pair_matrix = (same_map & (jnp.abs(row - column) == half // 2)).astype(jnp.bfloat16)
        for copy in copies:
            copy.wait()
        both_gains = [
            jnp.concatenate([ref[...], ref[...]], axis=1) for ref in (query_gain, key_gain)
        ]

        for part, gain in enumerate(both_gains):
            straight = cos_here[...] * gain
            crossed = sin_here[...] * pltpu.roll(gain, half // 2, 1)
            for group in range(groups):
                for head in range(plan.heads[group]):
                    field = staged[group][part, :, head * width : (head + 1) * width]
                    wide = field.astype(jnp.float32)
                    square = wide * wide
                    high = square.astype(jnp.bfloat16)
                    low = (square - high.astype(jnp.float32)).astype(jnp.bfloat16)
                    total = jnp.dot(
                        jnp.concatenate([high, low], axis=1), sum_twice, preferred_element_type=jnp.float32
                    )
                    pair = jnp.dot(field, pair_matrix, preferred_element_type=jnp.float32)
                    turned = wide * straight + pair * crossed
                    turned *= lax.rsqrt(total * (1.0 / half) + EPSILON)
                    own[group][part * plan.heads[group] + head] = turned.astype(jnp.bfloat16)
        for group in range(groups):
            for head in range(plan.heads[group]):
                own[group][VALUE * plan.heads[group] + head] = staged[group][
                    VALUE, :, head * width : (head + 1) * width
                ]

        for number, (_, members) in enumerate(plan.ins):
            for source, _, places in members:

                @pl.when(me == source)
                def _(number=number, places=places):
                    for (group, part), first in places:
                        skip = part * plan.heads[group]
                        count = 3 * plan.heads[group] - skip

                        def move(slab, carry, group=group, skip=skip, first=first):
                            buffers[number][first + slab] = own[group][skip + slab]
                            return carry

                        lax.fori_loop(0, count, move, 0, unroll=True)

    slabs = [3 * heads for heads in plan.heads] + [count for count, _ in plan.ins]
    results = pl.pallas_call(
        body,
        out_shape=[jax.ShapeDtypeStruct((count, tokens, width), jnp.bfloat16) for count in slabs],
        in_specs=[HBM_SPEC] * 7,
        out_specs=[VMEM_SPEC] * len(slabs),
        scratch_shapes=[pltpu.VMEM((3, tokens, heads * width), jnp.bfloat16) for heads in plan.heads]
        + [pltpu.VMEM((tokens, width), jnp.float32)] * 2
        + [pltpu.VMEM(gains[0].shape, jnp.float32)] * 2
        + [pltpu.SemaphoreType.DMA((4 + 3 * groups,))],
        compiler_params=pltpu.CompilerParams(vmem_limit_bytes=16 * MIB),
        name="pack",
    )(*rows, *tables, *gains)
    return results[:groups], results[groups:]


def attention(plan, own, arrived, lambdas, head_gain, first_heads):
    groups = len(plan.owners)
    tokens = own[0].shape[1]
    width = head_gain.shape[-1]
    half = width // 2
    exponent_scale = half ** (-0.5) * math.log2(math.e)
    unrolled = plan.n <= 4

    def body(lambda_ref, head_gain_ref, *refs):
        own_refs, refs = refs[:groups], refs[groups:]
        in_refs, refs = refs[: len(plan.ins)], refs[len(plan.ins) :]
        own_out, outs = refs[:groups], refs[groups:]
        me = lax.axis_index("sp")

        def block_of(device, group, part, head, slot):
            if slot == device:
                return own_refs[group][part * plan.heads[group] + head]
            lowest = QUERY if slot > plan.owners[group] else KEY
            number, first = plan.source_of(plan.ins, slot, device, (group, lowest))
            return in_refs[number][first + (part - lowest) * plan.heads[group] + head]

        def job(device, group, block, heads, gain, weight_of, store):
            slots = range(block + 1)
            first_map = lax.broadcasted_iota(jnp.int32, (tokens, width), 1) < half
            key_at = lax.broadcasted_iota(jnp.int32, (tokens, 2 * tokens), 0)
            query_at = lax.broadcasted_iota(jnp.int32, (tokens, 2 * tokens), 1) % tokens
            visible = key_at <= query_at

            maps, scores, values = [], [], []
            for head in heads:
                query = block_of(device, group, QUERY, head, block)
                zero = jnp.zeros_like(query)
                maps.append(
                    jnp.concatenate(
                        [jnp.where(first_map, query, zero), jnp.where(first_map, zero, query)], axis=0
                    )
                )
                values.append(
                    jnp.concatenate([block_of(device, group, VALUE, head, slot) for slot in slots], axis=0)
                )
            for head, query in zip(heads, maps):
                keys = jnp.concatenate([block_of(device, group, KEY, head, slot) for slot in slots], axis=0)
                product = lax.dot_general(
                    keys, query, (((1,), (1,)), ((), ())), preferred_element_type=jnp.float32
                )
                last = jnp.where(visible, product[block * tokens :], -1e30)
                scores.append(
                    jnp.concatenate([product[: block * tokens], last], axis=0) if block else last
                )
            highest = [jnp.max(part, axis=0, keepdims=True) for part in scores]
            exponents = [
                jnp.exp2((part - top) * exponent_scale) for part, top in zip(scores, highest)
            ]
            inverses = [1.0 / jnp.sum(part, axis=0, keepdims=True) for part in exponents]
            raws = []
            for head, exponent, inverse, value in zip(heads, exponents, inverses, values):
                mixing = (
                    exponent[:, :tokens] * inverse[:, :tokens]
                    - exponent[:, tokens:] * (inverse[:, tokens:] * weight_of(head))
                ).astype(jnp.bfloat16)
                raws.append(
                    lax.dot_general(
                        value, mixing, (((0,), (0,)), ((), ())), preferred_element_type=jnp.float32
                    )
                )
            for head, raw in zip(heads, raws):
                scaled = raw * lax.rsqrt(jnp.mean(raw * raw, axis=0, keepdims=True) + EPSILON)
                store(head, (scaled * gain).astype(jnp.bfloat16))

        for device, jobs in plan.jobs.items():
            if not jobs:
                continue

            @pl.when(me == device)
            def _(device=device, jobs=jobs):
                gain = jnp.transpose(
                    jnp.broadcast_to(head_gain_ref[...] * OUT_SCALE, (tokens, width))
                )
                for group, block in jobs:
                    if block == device:
                        target, first = own_out[group], 0
                    else:
                        number, first = plan.source_of(plan.outs, device, block, group)
                        target = outs[number]

                    def store(head, value, target=target, first=first):
                        target[first + head] = value

                    def weight_of(head, group=group):
                        return lambda_ref[first_heads[group] + head]

                    heads = plan.heads[group]
                    if unrolled:
                        job(device, group, block, range(heads), gain, weight_of, store)
                    else:

                        def one(head, carry, group=group, block=block, store=store, weight_of=weight_of):
                            job(device, group, block, [head], gain, weight_of, store)
                            return carry

                        lax.fori_loop(0, heads, one, 0)

    slabs = list(plan.heads) + [count for count, _ in plan.outs]
    results = pl.pallas_call(
        body,
        out_shape=[jax.ShapeDtypeStruct((count, width, tokens), jnp.bfloat16) for count in slabs],
        in_specs=[SMEM_SPEC] + [VMEM_SPEC] * (1 + groups + len(plan.ins)),
        out_specs=[VMEM_SPEC] * len(slabs),
        compiler_params=pltpu.CompilerParams(vmem_limit_bytes=(24 if unrolled else 48) * MIB),
        name="attend",
    )(lambdas, head_gain, *own, *arrived)
    return results[:groups], results[groups:]


def project(plan, own_heads, back, shards, total, first_heads, last, dtype):
    groups = len(plan.owners)
    _, width, tokens = own_heads[0].shape
    shard_columns = shards[0].shape[1]
    count = len(shards)
    given = 0 if total is None else 1
    starts = [sum(plan.heads[:group]) for group in range(groups)]

    def body(*refs):
        own_refs, refs = refs[:groups], refs[groups:]
        back_refs, refs = refs[: len(plan.outs)], refs[len(plan.outs) :]
        total_refs, refs = refs[:given], refs[given:]
        shard_refs, refs = refs[:count], refs[count:]
        out_ref, heads = refs
        me, column_place = lax.axis_index("sp"), lax.axis_index("dp")

        def take(ref, first, group):
            for head in range(plan.heads[group]):
                lanes = slice((starts[group] + head) * width, (starts[group] + head + 1) * width)
                heads[:, lanes] = jnp.transpose(ref[first + head])

        for group, owner in enumerate(plan.owners):
            pl.when(me <= owner)(functools.partial(take, own_refs[group], 0, group))
        for number, (_, members) in enumerate(plan.outs):
            for _, target, places in members:
                for group, first in places:
                    pl.when(me == target)(functools.partial(take, back_refs[number], first, group))

        for number in range(count):
            part = total_refs[0][number] if given else 0.0
            for group in range(groups):
                lanes = slice(starts[group] * width, (starts[group] + plan.heads[group]) * width)
                row = first_heads[group] * width
                part += jnp.dot(
                    heads[:, lanes],
                    shard_refs[number][row : row + plan.heads[group] * width, :],
                    preferred_element_type=jnp.float32,
                )
            if last:
                column = pl.multiple_of(shard_place(column_place, number, count) * shard_columns, shard_columns)
                out_ref[:, pl.ds(column, shard_columns)] = part.astype(dtype)
            else:
                out_ref[number] = part

    if last:
        out_shape = jax.ShapeDtypeStruct((tokens, count * shard_columns), dtype)
    else:
        out_shape = jax.ShapeDtypeStruct((count, tokens, shard_columns), jnp.float32)
    return pl.pallas_call(
        body,
        out_shape=out_shape,
        in_specs=[VMEM_SPEC] * (groups + len(plan.outs) + given + count),
        out_specs=VMEM_SPEC,
        scratch_shapes=[pltpu.VMEM((tokens, sum(plan.heads) * width), jnp.bfloat16)],
        compiler_params=pltpu.CompilerParams(vmem_limit_bytes=24 * MIB),
        name="project",
    )(*own_heads, *back, *([] if total is None else [total]), *shards)


def shard_place(place, number, count):
    if count & (count - 1) == 0:
        return jnp.bitwise_xor(place, number)
    return lax.rem(place + number, count)


def gather_shards(weight, hold):
    count = lax.axis_size("dp")
    if count & (count - 1):
        return [weight] + [
            lax.ppermute(weight, "dp", [(j, (j - k) % count) for j in range(count)])
            for k in range(1, count)
        ]
    shards, mask = {0: weight}, count // 2
    while mask:
        pairs = [(j, j ^ mask) for j in range(count)]
        sent = {}
        for k, shard in shards.items():
            sent[k ^ mask] = lax.ppermute(hold(shard) if k else shard, "dp", pairs)
        shards.update(sent)
        mask //= 2
    return [shards[k] for k in range(count)]


def rotation_tables(length, head_size):
    half_size = head_size // 2
    positions = np.arange(length, dtype=np.float32)
    inverse = np.float32(10000.0) ** (-np.arange(half_size, dtype=np.float32) / np.float32(half_size))
    angles = (positions[:, None] * inverse[None, :]).astype(np.float64)
    cosine_part, sine_part = np.cos(angles), np.sin(angles)
    return [
        in_hbm(jnp.asarray(np.concatenate(parts, axis=1).astype(np.float32)))
        for parts in ([cosine_part] * 4, [-sine_part, sine_part] * 2)
    ]


def bounds_of(heads):
    parts = len(CHUNK_PARTS)
    return [heads * sum(CHUNK_PARTS[:k]) // sum(CHUNK_PARTS) for k in range(parts + 1)]


def in_hbm(array):
    return pltpu.with_memory_space_constraint(array, pltpu.HBM)


def tie(array, other):
    return lax.optimization_barrier((array, other))[0]


def local(query_rows, key_rows, value_rows, query_gain, key_gain, lambdas, head_gain, out_weight):
    tokens = query_rows.shape[1]
    n = lax.axis_size("sp")
    owners = sorted({max(n // 2 - 1, 0), n // 2})
    heads_total = lambdas.shape[0]
    head_size, width = query_gain.shape[0], head_gain.shape[0]
    rows = [
        in_hbm(array.reshape(tokens, array.shape[2])) for array in (query_rows, key_rows, value_rows)
    ]
    first_count = max(1, int(heads_total * FIRST_GROUP)) if len(owners) > 1 else heads_total
    group_starts = [0, first_count][: len(owners)]
    group_bounds = [bounds_of(first_count), bounds_of(heads_total - first_count)][: len(owners)]
    chunks = []
    for k in range(len(CHUNK_PARTS)):
        heads = [bounds[k + 1] - bounds[k] for bounds in group_bounds]
        chunks.append(
            (Plan(n, owners, heads), [start + bounds[k] for start, bounds in zip(group_starts, group_bounds)])
        )

    tables = rotation_tables(tokens * n, head_size)
    gains = [in_hbm(gain.reshape(1, head_size)) for gain in (query_gain, key_gain)]
    head_gain = head_gain.reshape(1, width)
    own, arrived = [], []
    for plan, first_heads in chunks:
        if own:
            gains[0] = in_hbm(tie(gains[0], own[-1][0]))
        slabs, buffers = send_buffers(plan, rows, tables, gains, first_heads, width)
        own.append(slabs)
        arrived.append([lax.ppermute(buffer, "sp", pairs_of(flows)) for buffer, (_, flows) in zip(buffers, plan.ins)])
    attended = []
    for number, (plan, first_heads) in enumerate(chunks):
        head_gain = tie(head_gain, attended[-1][0][0] if attended else own[-1][0])
        own_heads, outward = attention(
            plan, own[number], arrived[number], lambdas, head_gain, first_heads
        )
        back = [
            lax.ppermute(buffer, "sp", pairs_of(flows)) for buffer, (_, flows) in zip(outward, plan.outs)
        ]
        attended.append((own_heads, back))
    shards = gather_shards(out_weight, lambda shard: tie(shard, attended[-1][0][0]))
    total = None
    for number, (plan, first_heads) in enumerate(chunks):
        total = project(
            plan, *attended[number], shards, total, first_heads, number == len(chunks) - 1, query_rows.dtype
        )
    return total.reshape(1, tokens, total.shape[1])


def solution(mesh):
    placed = (
        P(("grp", "dp"), "sp", None),
        P(("grp", "dp"), "sp", None),
        P(("grp", "dp"), "sp", None),
        P(),
        P(),
        P(),
        P(),
        P(None, "dp"),
    )

    return jax.shard_map(local, mesh=mesh, in_specs=placed, out_specs=P(("grp", "dp"), "sp", None), check_vma=False)
```
